32 devices in a mesh: kv: 8 (over z, x), tp: 4 (over y, core).
Axes of the slice: x: 2, y: 2, z: 4, core: 2. Of those that a mesh axis runs over, the one named last changes fastest.
Arguments:
- queries: bfloat16 [1024, 2048], P('kv', 'tp'), may hold values from -6 to 6
- keys: bfloat16 [1024, 2048], P('kv', 'tp'), may hold values from -6 to 6
- values: bfloat16 [1024, 2048], P('kv', 'tp'), may hold values from -6 to 6
- attended: bfloat16 [1024, 2048], P('kv', 'tp'), may hold values from -6 to 6
- cotangent: bfloat16 [1024, 2048], P('kv', 'tp'), may hold values from -96 to 96
- log_totals: float32 [32, 1024], P('tp', 'kv'), may hold values from 4 to 7
- block_picks: int32 [32, 16, 8], P('tp', 'kv'), may hold values from -1 to 14, as said below
- normed: bfloat16 [1024, 4096], P('kv', 'tp'), may hold values from -6 to 6
Outputs:
- grad_queries: bfloat16 [1024, 2048], P('kv', 'tp')
- grad_keys: bfloat16 [1024, 2048], P('kv', 'tp')
- grad_values: bfloat16 [1024, 2048], P('kv', 'tp')
- grad_weight: float32 [4096, 2048], P('kv', 'tp')
The draws below stay inside these ranges and needn't reach their ends.
Inputs may be any that keep to these rules, and one draw needn't show every extreme that they name: `block_picks`: row c of head h names at most 8 distinct blocks below c, followed by -1 in the other slots. One key block is named by at most 4 query blocks of one head, and in every draw each head has a block named exactly 4 times.
All inputs are finite; a program needn't handle non-finite values.
Results may differ from the reference program's by a relative error of at most 0.0069.
Values may be sent and summed in bfloat16 or wider, within the bound.
No kernel may reach another device: no remote copies, remote signals or barrier semaphores. Data moves between devices by JAX's collectives and lax.ppermute only.
A program may use at most 128 MiB of HBM per device.

```python
import jax
import jax.numpy as jnp
from jax import lax

D = 4096
H = 32
DH = 64
BLOCK = 64
SEL = 8
TOKENS = 1024
NQB = 16
MOST = 4


def draw_block_picks(key, part):
    key_jitter, key_hot = jax.random.split(jax.random.fold_in(key, 17))
    jitter = jax.random.randint(key_jitter, (H, NQB, NQB), 0, 2 ** 24 // NQB)
    hot_ids = jax.random.randint(key_hot, (H, 3), 0, max(1, NQB // 4))
    block_ids = jnp.arange(NQB)

    def one_head(jitter_h, hot_h):
        others = jnp.any(block_ids[:, None] == hot_h[None, 1:], axis=1)

        def advance(tallies, qblock):
            levels = jnp.where(others, 2, 1)
            levels = jnp.where(block_ids == qblock - NQB // 2, 3, levels)
            levels = jnp.where(block_ids == qblock - 1, 4, levels)
            levels = jnp.where(block_ids == hot_h[0], 5, levels)
            usable = (block_ids < qblock) & (tallies < MOST)
            scores = jnp.where(usable, levels * 2 ** 24 + jitter_h[qblock] * NQB + block_ids, -(block_ids + 1))
            top_vals, chosen_ids = lax.top_k(scores, SEL)
            row_ids = jnp.where(top_vals >= 0, chosen_ids, -1).astype(jnp.int32)
            tallies = tallies + jnp.sum((row_ids[:, None] == block_ids[None, :]).astype(jnp.int32), axis=0)
            return (tallies, row_ids)
        _, table = lax.scan(advance, jnp.zeros((NQB,), jnp.int32), jnp.arange(NQB))
        return table
    return jax.vmap(one_head)(jitter, hot_ids).astype(jnp.int32)


def spiked(entries, key, source, target, parts, factor):
    def block_of(dim):
        return (jnp.arange(entries.shape[dim]) // (entries.shape[dim] // parts)).reshape((-1,) + (1,) * (entries.ndim - 1 - dim))

    one_side = jax.random.permutation(key, parts)[block_of(target)]
    other_side = (block_of(target) + parts // 2) % parts
    return jnp.where((block_of(source) == one_side) | (block_of(source) == other_side), factor * entries, entries)


def block_levels(rng, shape, cuts, smallest, high):
    def one(position, blocks):
        steps = jax.random.uniform(jax.random.fold_in(jax.random.fold_in(rng, 6), position), (blocks,), jnp.float32, smallest / len(cuts), high / len(cuts))
        return jnp.repeat(jnp.exp(steps), shape[position] // blocks).reshape((-1,) + (1,) * (len(shape) - position - 1))

    loudness = one(*cuts[0])
    for cut in cuts[1:]:
        loudness = loudness * one(*cut)
    return loudness


def centred(stream_key, shape, width, most, shards=(), held_as=jnp.bfloat16):
    values = width * jax.random.normal(stream_key, shape, jnp.float32)
    if shards:
        values = values * block_levels(stream_key, shape, shards, -0.22, 0.18)
    return jnp.clip(values, -most, most).astype(held_as)


def heavy_noise(rng, extent, scale, limit, cuts, heavy, kind=jnp.bfloat16):
    result = scale * jax.random.normal(rng, extent, jnp.float32)
    if cuts:
        result = result * block_levels(rng, extent, cuts, -0.22, 0.18)
    return jnp.clip(spiked(result, jax.random.fold_in(rng, 3), *heavy), -limit, limit).astype(kind)


def setup_inputs(seed: int = 0) -> dict:
    splits = jax.random.split(jax.random.key(seed), 9)
    queries = centred(splits[0], (TOKENS, H * DH), 1.0, 6.0, ((0, 8), (1, 4)))
    keys = centred(splits[1], (TOKENS, H * DH), 1.0, 6.0, ((0, 8), (1, 4)))
    values = centred(splits[2], (TOKENS, H * DH), 1.0, 6.0, ((0, 8), (1, 4)))
    attended = centred(splits[3], (TOKENS, H * DH), 1.0, 6.0, ((0, 8), (1, 4)))
    cotangent = centred(splits[4], (TOKENS, H * DH), 16.0, 96.0, ((0, 8), (1, 4)))
    log_totals = jnp.clip(4.0 + 3.0 * jax.random.uniform(splits[5], (H, TOKENS), jnp.float32) ** block_levels(splits[5], (H, TOKENS), ((0, 4), (1, 8)), -0.2, 0.2), 4.0, 7.0)
    block_picks = draw_block_picks(jax.random.fold_in(splits[8], 71), 0)
    normed = heavy_noise(splits[7], (TOKENS, D), 1.0, 6.0, ((0, 8), (1, 4)), (0, 1, 8, 2.0))
    return {"queries": queries, "keys": keys, "values": values, "attended": attended, "cotangent": cotangent, "log_totals": log_totals, "block_picks": block_picks, "normed": normed}


def tile_grads(q_tile, k_tile, v_tile, g_tile, log_total, row_dots, allowed):
    scale = q_tile.shape[-1] ** -0.5
    scores = jnp.einsum('...qd,...kd->...qk', q_tile, k_tile) * scale
    probs = jnp.where(allowed, jnp.exp(scores - log_total[..., None]), 0.0)
    probs_low = lax.optimization_barrier(probs.astype(jnp.bfloat16)).astype(jnp.float32)
    grad_v = jnp.einsum('...qk,...qd->...kd', probs_low, g_tile)
    grad_p = jnp.einsum('...qd,...kd->...qk', g_tile, v_tile)
    grad_s = (probs * (grad_p - row_dots[..., None])).astype(jnp.bfloat16)
    grad_s = lax.optimization_barrier(grad_s).astype(jnp.float32)
    grad_q = jnp.einsum('...qk,...kd->...qd', grad_s, k_tile) * scale
    grad_k = jnp.einsum('...qk,...qd->...kd', grad_s, q_tile) * scale
    return grad_q, grad_k, grad_v


def by_head(matrix):
    return matrix.astype(jnp.float32).reshape(NQB, BLOCK, H, DH).transpose(2, 0, 1, 3)


def to_rows(tensor):
    return tensor.transpose(1, 2, 0, 3).reshape(NQB * BLOCK, H * DH)


def reference(queries, keys, values, attended, cotangent, log_totals, block_picks, normed):
    causal = jnp.tril(jnp.ones((BLOCK, BLOCK), bool))
    log_heads = log_totals.reshape(H, NQB, BLOCK)

    def per_head(operands):
        q_h, k_h, v_h, o_h, g_h, l_h, picked = operands
        row_dots = jnp.sum(g_h * o_h, axis=-1)
        dq_diag, dk_diag, dv_diag = tile_grads(q_h, k_h, v_h, g_h, l_h, row_dots, causal)
        present = picked >= 0
        clamped = jnp.maximum(picked, 0)
        k_sel = k_h[clamped]
        v_sel = v_h[clamped]
        tile_shape = k_sel.shape
        q_rep = jnp.broadcast_to(q_h[:, None], tile_shape)
        g_rep = jnp.broadcast_to(g_h[:, None], tile_shape)
        l_rep = jnp.broadcast_to(l_h[:, None], tile_shape[:3])
        d_rep = jnp.broadcast_to(row_dots[:, None], tile_shape[:3])
        allowed = jnp.broadcast_to(present[:, :, None, None], tile_shape[:3] + (BLOCK,))
        dq_sel, dk_sel, dv_sel = tile_grads(q_rep, k_sel, v_sel, g_rep, l_rep, d_rep, allowed)
        segments = jnp.where(present, picked, NQB).reshape(-1).astype(jnp.int32)
        dk_sum = jax.ops.segment_sum(dk_sel.reshape(-1, BLOCK, DH), segments, num_segments=NQB + 1)[:NQB]
        dv_sum = jax.ops.segment_sum(dv_sel.reshape(-1, BLOCK, DH), segments, num_segments=NQB + 1)[:NQB]
        return dq_diag + jnp.sum(dq_sel, axis=1), dk_diag + dk_sum, dv_diag + dv_sum

    grad_q, grad_k, grad_v = lax.map(per_head, (by_head(queries), by_head(keys), by_head(values),
                                                by_head(attended), by_head(cotangent), log_heads, block_picks))
    grad_queries = to_rows(grad_q).astype(jnp.bfloat16)
    grad_weight = jnp.dot(normed.T, grad_queries, preferred_element_type=jnp.float32)
    return grad_queries, to_rows(grad_k).astype(jnp.bfloat16), to_rows(grad_v).astype(jnp.bfloat16), grad_weight
```

```python
import functools
import math

import jax
import jax.numpy as jnp
from jax import lax
from jax.experimental import pallas as pl
from jax.experimental.pallas import tpu as pltpu
from jax.sharding import PartitionSpec as P

BLOCK = 64
LANES = 128
AUX = 16
MASKED = -1e30

BF16 = jnp.bfloat16
F32 = jnp.float32
NN = (((1,), (0,)), ((), ()))
NT = (((1,), (1,)), ((), ()))


def dot(a, b, dims, **kw):
    return lax.dot_general(a, b, dims, preferred_element_type=F32, **kw)


def three_parts(x):
    hi = x.astype(BF16)
    rest = x - hi.astype(F32)
    mid = rest.astype(BF16)
    return hi, mid, (rest - mid.astype(F32)).astype(BF16)


def turned(x):
    return x.astype(F32).T.astype(BF16)


def pack_kernel(heads, me_ref, picks_ref, q_ref, k_ref, v_ref, g_ref, o_ref, log_ref, *rest):
    outs, held = rest[:-1], rest[-1]
    rows, width = q_ref.shape
    size = width // heads
    slots = picks_ref.shape[-1]
    prods = three_parts(g_ref[...].astype(F32) * o_ref[...].astype(F32))
    head_id = lax.broadcasted_iota(jnp.int32, (heads, width), 0)
    col_head = lax.broadcasted_iota(jnp.int32, (heads, width), 1) // size
    ones = jnp.where(head_id == col_head, 1.0, 0.0).astype(BF16)
    dots = dot(ones, prods[0], NT) + dot(ones, prods[1], NT) + dot(ones, prods[2], NT)
    log_parts = [p.astype(F32) for p in three_parts(log_ref[...])]
    dot_parts = [p.astype(F32) for p in three_parts(dots)]
    lane = lax.broadcasted_iota(jnp.int32, (1, rows), 1)
    half = lax.broadcasted_iota(jnp.int32, (rows, LANES), 1) < size
    for pair in range(width // LANES):
        cols = pl.ds(pair * LANES, LANES)
        q_t = turned(q_ref[:, cols])
        g_t = turned(g_ref[:, cols])
        k_pair = k_ref[:, cols].astype(F32)
        v_pair = v_ref[:, cols].astype(F32)
        for side in range(LANES // size):
            head = pair * (LANES // size) + side
            held[head, 0:size, :] = q_t[side * size : (side + 1) * size]
            held[head, size : 2 * size, :] = g_t[side * size : (side + 1) * size]
            if side == 0:
                both = jnp.where(half, k_pair, pltpu.roll(v_pair, size, 1))
            else:
                both = jnp.where(half, pltpu.roll(k_pair, size, 1), v_pair)
            held[head, 2 * size : 2 * size + rows, :] = both.astype(BF16)
            aux = [p[head : head + 1] for p in log_parts + dot_parts]
            for s in range(slots):
                name = jnp.full((1, rows), picks_ref[head, 0, s], jnp.int32)
                for c in range(1, rows // BLOCK):
                    name = jnp.where(lane >= c * BLOCK, picks_ref[head, c, s], name)
                aux.append(name.astype(F32))
            aux.append(jnp.zeros((AUX - len(aux), rows), F32))
            held[head, 2 * size + rows :, :] = jnp.concatenate(aux, axis=0).astype(BF16)
    me = me_ref[0]
    for r, out in enumerate(outs):
        out[...] = held[lax.rem(me ^ r, heads)]


def head_kernel(heads, blocks, slots, me_ref, *rest):
    n = (len(rest) - heads - 6)
    msgs, outs = rest[:n], rest[n : n + heads]
    kv_ext, k_t, rhs, q_rows, dkv, dq = rest[n + heads :]
    size = BLOCK
    rows = LANES
    me = me_ref[0]
    chunks = n
    scale = size ** (-0.5)
    ext = kv_ext.shape[1] - LANES
    lane = lax.broadcasted_iota(jnp.int32, (rows, ext), 1)
    sub = lax.broadcasted_iota(jnp.int32, (rows, ext), 0)
    block_row = lax.broadcasted_iota(jnp.int32, (blocks, rows), 0)
    q_lane = lax.broadcasted_iota(jnp.int32, (blocks, rows), 1)
    per = rows // BLOCK
    zeros = jnp.zeros((size, rows), BF16)
    pad = jnp.zeros((ext - blocks - AUX, rows), BF16)
    lead = jnp.zeros((blocks, rows), BF16)
    part = lax.broadcasted_iota(jnp.int32, (AUX, rows), 0)
    for r in range(chunks):
        src = me ^ r
        at = pl.ds(pl.multiple_of(src * rows, rows), rows)
        q_t = msgs[r][0:size, :]
        g_t = msgs[r][size : 2 * size, :]
        both = msgs[r][2 * size : 2 * size + rows, :]
        aux = msgs[r][2 * size + rows :, :].astype(F32)
        own_block = src * per + sub // BLOCK
        ext_val = jnp.where(lane < blocks, jnp.where(lane == own_block, 1.0, 0.0), jnp.where(lane < blocks + 3, 1.0, 0.0))
        kv_ext[at, 0:LANES] = both
        kv_ext[at, LANES:] = ext_val.astype(BF16)
        k_t[:, at] = both.astype(F32).T[0:size].astype(BF16)
        admit = block_row == src * per + q_lane // BLOCK
        for s in range(slots):
            admit = admit | (block_row == aux[6 + s : 7 + s].astype(jnp.int32))
        bias = jnp.where(admit, 0.0, MASKED).astype(BF16)
        log_rows = jnp.where(part < 3, aux * (-1.0 / scale), 0.0).astype(BF16)
        dot_rows = jnp.where(part < 3, -pltpu.roll(aux, AUX - 3, 0), 0.0).astype(BF16)
        q_rows[:, at] = msgs[r][0 : 2 * size, :]
        rhs[0, :, at] = jnp.concatenate([q_t, zeros, bias, log_rows, pad], axis=0)
        rhs[1, :, at] = jnp.concatenate([zeros, g_t, lead, dot_rows, pad], axis=0)
    dkv[...] = jnp.zeros(dkv.shape, F32)
    dq[...] = jnp.zeros(dq.shape, F32)
    tile = min(2 * LANES, chunks * rows)
    tiles = chunks * rows // tile
    gain = scale * math.log2(math.e)
    k_pos = lax.broadcasted_iota(jnp.int32, (tile, tile), 0)
    q_pos = lax.broadcasted_iota(jnp.int32, (tile, tile), 1)
    ahead = k_pos > q_pos

    def one(qc, kb, diag):
        qs = pl.ds(pl.multiple_of(qc * tile, tile), tile)
        ks = pl.ds(pl.multiple_of(kb * tile, tile), tile)
        left = kv_ext[ks, :]
        probs = jnp.exp2(dot(left, rhs[0, :, qs], NN) * gain)
        if diag:
            probs = jnp.where(ahead, 0.0, probs)
        grad_p = dot(left, rhs[1, :, qs], NN)
        grad_s = (probs * grad_p).astype(BF16)
        dkv[0, ks, :] += dot(grad_s, q_rows[0:size, qs], NT)
        dkv[1, ks, :] += dot(probs.astype(BF16), q_rows[size:, qs], NT)
        dq[:, qs] += dot(k_t[:, ks], grad_s, NN)

    if tiles <= 4:
        for qc in range(tiles):
            for kb in range(qc + 1):
                one(qc, kb, kb == qc)
    else:
        @pl.loop(0, tiles)
        def _(qc):
            @pl.loop(0, qc)
            def _(kb):
                one(qc, kb, False)

            one(qc, qc, True)

    for r, out in enumerate(outs):
        at = pl.ds(pl.multiple_of((me ^ r) * rows, rows), rows)
        for c in range(chunks):
            out[c * size : (c + 1) * size, :] = (dq[:, c * rows : (c + 1) * rows] * scale).astype(BF16)
        out[chunks * size :, :] = jnp.concatenate(
            [dkv[0, at, :] * scale, dkv[1, at, :]], axis=1
        ).astype(BF16)


def turn_kernel(spread, me_ref, kept_ref, *rest):
    others, out = rest[:-1], rest[-1]
    rows = kept_ref.shape[0]
    width = out.shape[0]
    mine = lax.rem(me_ref[0], spread)
    for r in range(spread):
        if r == 0:
            piece = kept_ref[:, pl.ds(pl.multiple_of(mine * width, width), width)]
        else:
            piece = others[r - 1][...]
        at = pl.ds(pl.multiple_of((mine ^ r) * rows, rows), rows)
        out[:, at] = turned(piece)


def final_kernel(heads, groups, me_ref, tp_ref, *rest):
    gots, normed, outs = rest[:heads], rest[heads : heads + groups], rest[heads + groups : heads + groups + 4]
    dq, pairs = rest[heads + groups + 4 :]
    grad_q, grad_k, grad_v, grad_w = outs
    rows = LANES
    size = BLOCK
    me = me_ref[0]
    span = dq.shape[2]
    chunks = (gots[0].shape[0] - rows) // size
    per = span // rows
    for r in range(heads):
        head = lax.rem(me ^ r, heads)
        at = pl.ds(pl.multiple_of(head * size, size), size)
        for c in range(chunks):
            dq[c // per, at, (c % per) * rows : (c % per + 1) * rows] = gots[r][c * size : (c + 1) * size, :]
        pairs[head] = gots[r][chunks * size :, :]
    total = None
    for r in range(groups):
        term = dot(normed[r][...], dq[tp_ref[0] ^ r], NT)
        total = term if total is None else total + term
    grad_w[...] = total
    half = lax.broadcasted_iota(jnp.int32, (rows, LANES), 1) < size
    own = pl.ds(pl.multiple_of(lax.rem(me, per) * rows, rows), rows)
    for p in range(heads * size // LANES):
        cols = pl.ds(p * LANES, LANES)
        grad_q[:, cols] = turned(dq[me // per, p * LANES : (p + 1) * LANES, own])
        a = pairs[2 * p].astype(F32)
        b = pairs[2 * p + 1].astype(F32)
        grad_k[:, cols] = jnp.where(half, a, pltpu.roll(b, size, 1)).astype(BF16)
        grad_v[:, cols] = jnp.where(half, pltpu.roll(a, size, 1), b).astype(BF16)


def smem():
    return pl.BlockSpec(memory_space=pltpu.SMEM)


def vmem():
    return pl.BlockSpec(memory_space=pltpu.VMEM)


def local(queries, keys, values, attended, cotangent, log_totals, block_picks, normed):
    rows, width = queries.shape
    heads = log_totals.shape[0]
    size = width // heads
    kv = lax.axis_size("kv")
    tp = lax.axis_size("tp")
    spread = kv // tp
    blocks = kv * rows // BLOCK
    assert rows == LANES and size == BLOCK and kv % heads == 0 and kv % tp == 0
    me = lax.axis_index("kv").reshape(1)
    mine_tp = lax.axis_index("tp").reshape(1)

    def to_kv(x, r):
        return lax.ppermute(x, "kv", [(i, i ^ r) for i in range(kv)])

    def to_tp(x, r):
        return lax.ppermute(x, "tp", [(i, i ^ r) for i in range(tp)])

    depth = 2 * size + rows + AUX
    packed = pl.pallas_call(
        functools.partial(pack_kernel, heads),
        out_shape=[jax.ShapeDtypeStruct((depth, rows), BF16)] * kv,
        in_specs=[smem(), smem()] + [vmem()] * 6,
        out_specs=[vmem()] * kv,
        scratch_shapes=[pltpu.VMEM((heads, depth, rows), BF16)],
        name="pack",
    )(me, block_picks, queries, keys, values, cotangent, attended, log_totals)
    msgs = [packed[0]] + [to_kv(packed[r], r) for r in range(1, kv)]

    pairs = [
        ((a * spread + b) * tp + j, (j * spread + b) * tp + a)
        for a in range(tp)
        for b in range(spread)
        for j in range(tp)
    ]
    swapped = lax.ppermute(normed, ("kv", "tp"), pairs)
    part = swapped.shape[1] // spread
    fine = lax.rem(me[0], spread)
    others = [
        to_kv(lax.dynamic_slice_in_dim(swapped, (fine ^ r) * part, part, axis=1), r)
        for r in range(1, spread)
    ]
    gathered = [
        pl.pallas_call(
            functools.partial(turn_kernel, spread),
            out_shape=jax.ShapeDtypeStruct((part, spread * rows), BF16),
            in_specs=[smem()] + [vmem()] * spread,
            out_specs=vmem(),
            name="turn",
        )(me, swapped, *others)
    ]
    r = tp // 2
    slots = [0]
    while r:
        gathered += [to_tp(x, r) for x in gathered]
        slots += [s ^ r for s in slots]
        r //= 2
    gathered = [gathered[slots.index(s)] for s in range(tp)]

    ext = LANES * (-(-(blocks + AUX) // LANES))
    total = kv * rows
    sent = pl.pallas_call(
        functools.partial(head_kernel, heads, blocks, block_picks.shape[-1]),
        out_shape=[jax.ShapeDtypeStruct((kv * size + rows, LANES), BF16)] * heads,
        in_specs=[smem()] + [vmem()] * kv,
        out_specs=[vmem()] * heads,
        scratch_shapes=[
            pltpu.VMEM((total, LANES + ext), BF16),
            pltpu.VMEM((size, total), BF16),
            pltpu.VMEM((2, LANES + ext, total), BF16),
            pltpu.VMEM((2 * size, total), BF16),
            pltpu.VMEM((2, total, size), F32),
            pltpu.VMEM((size, total), F32),
        ],
        name="head",
    )(me, *msgs)
    gots = [sent[0]] + [to_kv(sent[r], r) for r in range(1, heads)]

    return pl.pallas_call(
        functools.partial(final_kernel, heads, tp),
        out_shape=[jax.ShapeDtypeStruct((rows, width), BF16)] * 3
        + [jax.ShapeDtypeStruct((part, width), F32)],
        in_specs=[smem(), smem()] + [vmem()] * (heads + tp),
        out_specs=[vmem()] * 4,
        scratch_shapes=[
            pltpu.VMEM((tp, heads * size, total // tp), BF16),
            pltpu.VMEM((heads, rows, LANES), BF16),
        ],
        name="final",
    )(me, mine_tp, *gots, *gathered)


def solution(mesh):
    in_specs = (
        P("kv", "tp"),
        P("kv", "tp"),
        P("kv", "tp"),
        P("kv", "tp"),
        P("kv", "tp"),
        P("tp", "kv"),
        P("tp", "kv", None),
        P("kv", "tp"),
    )
    out_specs = (P("kv", "tp"), P("kv", "tp"), P("kv", "tp"), P("kv", "tp"))

    def step(*args):
        return tuple(local(*args))

    return jax.shard_map(step, mesh=mesh, in_specs=in_specs, out_specs=out_specs, check_vma=False)
```

```python
import functools
import math

import jax
import jax.numpy as jnp
from jax import lax
from jax.experimental import pallas as pl
from jax.experimental.pallas import tpu as pltpu
from jax.sharding import PartitionSpec as P


BLOCK = 64
LANES = 128
AUX = 16
GRANT = 32 * 1024 * 1024
MASKED = -1e30

BF16 = jnp.bfloat16
F32 = jnp.float32
NN = (((1,), (0,)), ((), ()))
NT = (((1,), (1,)), ((), ()))


def dot(a, b, dims, **kw):
    return lax.dot_general(a, b, dims, preferred_element_type=F32, **kw)


def three_parts(x):
    hi = x.astype(BF16)
    rest = x - hi.astype(F32)
    mid = rest.astype(BF16)
    return hi, mid, (rest - mid.astype(F32)).astype(BF16)


def turned(x):
    return x.astype(F32).T.astype(BF16)


def pack_kernel(heads, each, me_ref, picks_ref, q_ref, k_ref, v_ref, g_ref, o_ref, log_ref, *rest):
    outs, held = rest[:-1], rest[-1]
    rows, width = q_ref.shape
    size = width // heads
    slots = picks_ref.shape[-1]
    prods = three_parts(g_ref[...].astype(F32) * o_ref[...].astype(F32))
    head_id = lax.broadcasted_iota(jnp.int32, (heads, width), 0)
    col_head = lax.broadcasted_iota(jnp.int32, (heads, width), 1) // size
    ones = jnp.where(head_id == col_head, 1.0, 0.0).astype(BF16)
    dots = dot(ones, prods[0], NT) + dot(ones, prods[1], NT) + dot(ones, prods[2], NT)
    log_parts = [p.astype(F32) for p in three_parts(log_ref[...])]
    dot_parts = [p.astype(F32) for p in three_parts(dots)]
    lane = lax.broadcasted_iota(jnp.int32, (1, rows), 1)
    half = lax.broadcasted_iota(jnp.int32, (rows, LANES), 1) < size
    for pair in range(width // LANES):
        cols = pl.ds(pair * LANES, LANES)
        q_t = turned(q_ref[:, cols])
        g_t = turned(g_ref[:, cols])
        k_pair = k_ref[:, cols].astype(F32)
        v_pair = v_ref[:, cols].astype(F32)
        for side in range(LANES // size):
            head = pair * (LANES // size) + side
            held[head, 0:size, :] = q_t[side * size : (side + 1) * size]
            held[head, size : 2 * size, :] = g_t[side * size : (side + 1) * size]
            if side == 0:
                both = jnp.where(half, k_pair, pltpu.roll(v_pair, size, 1))
            else:
                both = jnp.where(half, pltpu.roll(k_pair, size, 1), v_pair)
            held[head, 2 * size : 2 * size + rows, :] = both.astype(BF16)
            aux = [p[head : head + 1] for p in log_parts + dot_parts]
            for s in range(slots):
                name = jnp.full((1, rows), picks_ref[head, 0, s], jnp.int32)
                for c in range(1, rows // BLOCK):
                    name = jnp.where(lane >= c * BLOCK, picks_ref[head, c, s], name)
                aux.append(name.astype(F32))
            aux.append(jnp.zeros((AUX - len(aux), rows), F32))
            held[head, 2 * size + rows :, :] = jnp.concatenate(aux, axis=0).astype(BF16)
    me = me_ref[0]
    for r, out in enumerate(outs):
        first = lax.rem(me ^ r, heads // each) * each
        for n in range(each):
            out[n] = held[first + n]


def head_kernel(group, blocks, slots, me_ref, *rest):
    count = len(rest) - group - 5
    msgs, outs = rest[:count], rest[count : count + group]
    kv_ext, k_t, rhs, dkv, dq = rest[count + group :]
    each = msgs[0].shape[0]
    size = BLOCK
    rows = LANES
    me = me_ref[0]
    scale = size ** (-0.5)
    ext = kv_ext.shape[2] - LANES
    lane = lax.broadcasted_iota(jnp.int32, (rows, ext), 1)
    sub = lax.broadcasted_iota(jnp.int32, (rows, ext), 0)
    block_row = lax.broadcasted_iota(jnp.int32, (blocks, rows), 0)
    q_lane = lax.broadcasted_iota(jnp.int32, (blocks, rows), 1)
    per = rows // BLOCK
    zeros = jnp.zeros((size, rows), BF16)
    pad = jnp.zeros((ext - blocks - AUX, rows), BF16)
    lead = jnp.zeros((blocks, rows), BF16)
    part = lax.broadcasted_iota(jnp.int32, (AUX, rows), 0)
    for r in range(count):
        src = me ^ r
        at = pl.ds(pl.multiple_of(src * rows, rows), rows)
        own_block = src * per + sub // BLOCK
        ones = (lane >= blocks) & (lane < blocks + 3)
        ext_val = jnp.where((lane == own_block) | ones, 1.0, 0.0).astype(BF16)
        for n in range(each):
            q_t = msgs[r][n, 0:size, :]
            g_t = msgs[r][n, size : 2 * size, :]
            both = msgs[r][n, 2 * size : 2 * size + rows, :]
            aux = msgs[r][n, 2 * size + rows :, :].astype(F32)
            kv_ext[n, at, 0:LANES] = both
            kv_ext[n, at, LANES:] = ext_val
            k_t[n, :, at] = both.astype(F32).T[0:size].astype(BF16)
            admit = block_row == src * per + q_lane // BLOCK
            for s in range(slots):
                admit = admit | (block_row == aux[6 + s : 7 + s].astype(jnp.int32))
            bias = jnp.where(admit, 0.0, MASKED).astype(BF16)
            log_rows = jnp.where(part < 3, aux * (-1.0 / scale), 0.0).astype(BF16)
            dot_rows = jnp.where(part < 3, -pltpu.roll(aux, AUX - 3, 0), 0.0).astype(BF16)
            rhs[n, 0, :, at] = jnp.concatenate([q_t, zeros, bias, log_rows, pad], axis=0)
            rhs[n, 1, :, at] = jnp.concatenate([zeros, g_t, lead, dot_rows, pad], axis=0)
    tile = min(2 * LANES, count * rows)
    tiles = count * rows // tile
    gain = scale * math.log2(math.e)
    k_pos = lax.broadcasted_iota(jnp.int32, (tile, tile), 0)
    q_pos = lax.broadcasted_iota(jnp.int32, (tile, tile), 1)
    ahead = k_pos > q_pos

    def span(i):
        return pl.ds(pl.multiple_of(i * tile, tile), tile)

    def one(n, qc, kb, diag):
        qs, ks = span(qc), span(kb)
        left = kv_ext[n, ks, :]
        probs = jnp.exp2(dot(left, rhs[n, 0, :, qs], NN) * gain)
        if diag:
            probs = jnp.where(ahead, 0.0, probs)
        grad_p = dot(left, rhs[n, 1, :, qs], NN)
        grad_s = (probs * grad_p).astype(BF16)
        kv_term = dot(grad_s, rhs[n, 0, 0:LANES, qs], NT) + dot(probs.astype(BF16), rhs[n, 1, 0:LANES, qs], NT)
        return kv_term, dot(k_t[n, :, ks], grad_s, NN)

    if tiles <= 4:
        for n in range(each):
            for qc in range(tiles):
                q_sum = None
                for kb in range(qc + 1):
                    kv_term, q_term = one(n, qc, kb, kb == qc)
                    q_sum = q_term if q_sum is None else q_sum + q_term
                    if kb == qc:
                        dkv[n, span(kb), :] = kv_term
                    else:
                        dkv[n, span(kb), :] += kv_term
                dq[n, :, span(qc)] = (q_sum * scale).astype(BF16)
    else:
        for n in range(each):
            dkv[n] = jnp.zeros(dkv.shape[1:], F32)

            @pl.loop(0, tiles)
            def _(qc):
                def below(kb, q_sum):
                    kv_term, q_term = one(n, qc, kb, False)
                    dkv[n, span(kb), :] += kv_term
                    return q_sum + q_term

                q_sum = lax.fori_loop(0, qc, below, jnp.zeros((size, tile), F32))
                kv_term, q_term = one(n, qc, qc, True)
                dkv[n, span(qc), :] += kv_term
                dq[n, :, span(qc)] = ((q_sum + q_term) * scale).astype(BF16)

    factor = jnp.where(lax.broadcasted_iota(jnp.int32, (rows, LANES), 1) < size, scale, 1.0)
    for r, out in enumerate(outs):
        at = pl.ds(pl.multiple_of((me ^ r) * rows, rows), rows)
        for n in range(each):
            for c in range(count):
                out[n, c * size : (c + 1) * size, :] = dq[n, :, c * rows : (c + 1) * rows]
            out[n, count * size :, :] = (dkv[n, at, :] * factor).astype(BF16)


def turn_kernel(spread, me_ref, kept_ref, *rest):
    others, out = rest[:-1], rest[-1]
    rows = kept_ref.shape[0]
    width = out.shape[0]
    mine = lax.rem(me_ref[0], spread)
    for r in range(spread):
        if r == 0:
            piece = kept_ref[:, pl.ds(pl.multiple_of(mine * width, width), width)]
        else:
            piece = others[r - 1][...]
        at = pl.ds(pl.multiple_of((mine ^ r) * rows, rows), rows)
        out[:, at] = turned(piece)


def final_kernel(group, groups, me_ref, tp_ref, *rest):
    gots, normed, outs = rest[:group], rest[group : group + groups], rest[group + groups : group + groups + 4]
    dq, pairs = rest[group + groups + 4 :]
    grad_q, grad_k, grad_v, grad_w = outs
    rows = LANES
    size = BLOCK
    me = me_ref[0]
    each = gots[0].shape[0]
    span = dq.shape[2]
    chunks = (gots[0].shape[1] - rows) // size
    per = span // rows
    for r in range(group):
        first = lax.rem(me ^ r, group) * each
        for n in range(each):
            at = pl.ds(pl.multiple_of((first + n) * size, size), size)
            for c in range(chunks):
                dq[c // per, at, (c % per) * rows : (c % per + 1) * rows] = gots[r][n, c * size : (c + 1) * size, :]
            pairs[first + n] = gots[r][n, chunks * size :, :]
    total = None
    for r in range(groups):
        term = dot(normed[r][...], dq[tp_ref[0] ^ r], NT)
        total = term if total is None else total + term
    grad_w[...] = total
    half = lax.broadcasted_iota(jnp.int32, (rows, LANES), 1) < size
    own = pl.ds(pl.multiple_of(lax.rem(me, per) * rows, rows), rows)
    for p in range(group * each * size // LANES):
        cols = pl.ds(p * LANES, LANES)
        grad_q[:, cols] = turned(dq[me // per, p * LANES : (p + 1) * LANES, own])
        a = pairs[2 * p].astype(F32)
        b = pairs[2 * p + 1].astype(F32)
        grad_k[:, cols] = jnp.where(half, a, pltpu.roll(b, size, 1)).astype(BF16)
        grad_v[:, cols] = jnp.where(half, pltpu.roll(a, size, 1), b).astype(BF16)


def held_in_vmem(xs):
    return [pltpu.with_memory_space_constraint(x, pltpu.VMEM) for x in xs]


def call(kernel, n_smem, n_in, out_shape, scratch=(), grant=GRANT):
    single = not isinstance(out_shape, list)
    return pl.pallas_call(
        kernel,
        out_shape=out_shape,
        in_specs=[pl.BlockSpec(memory_space=pltpu.SMEM)] * n_smem + [pl.BlockSpec(memory_space=pltpu.VMEM)] * n_in,
        out_specs=pl.BlockSpec(memory_space=pltpu.VMEM)
        if single
        else [pl.BlockSpec(memory_space=pltpu.VMEM)] * len(out_shape),
        scratch_shapes=list(scratch),
        compiler_params=pltpu.CompilerParams(vmem_limit_bytes=grant),
    )


def group_size(kv, heads):
    return min(heads, max(kv // 2, 1))


def local(queries, keys, values, attended, cotangent, log_totals, block_picks, normed):
    rows, width = queries.shape
    heads = log_totals.shape[0]
    size = width // heads
    slots = block_picks.shape[-1]
    kv = lax.axis_size("kv")
    tp = lax.axis_size("tp")
    spread = kv // tp
    group = group_size(kv, heads)
    each = heads // group
    blocks = kv * rows // BLOCK
    assert rows == LANES and size == BLOCK and 6 + slots <= AUX
    assert kv % group == 0 and heads % group == 0 and kv % tp == 0
    me = lax.axis_index("kv").reshape(1)
    mine_tp = lax.axis_index("tp").reshape(1)

    def to_kv(x, r):
        return lax.ppermute(x, "kv", [(i, i ^ r) for i in range(kv)])

    def to_tp(x, r):
        return lax.ppermute(x, "tp", [(i, i ^ r) for i in range(tp)])

    part = normed.shape[1] // spread
    fine = lax.rem(me[0], spread)
    cuts = [
        lax.dynamic_slice_in_dim(normed, (fine ^ r) * part, part, axis=1) for r in range(1, spread)
    ]
    others = [to_kv(c, r + 1) for r, c in enumerate(cuts)]
    piece = call(
        functools.partial(turn_kernel, spread), 1, spread, pltpu.VMEM((part, spread * rows), BF16), (), None
    )(me, normed, *held_in_vmem(others))
    pairs = [
        ((a * spread + b) * tp + j, (j * spread + b) * tp + a)
        for a in range(tp)
        for b in range(spread)
        for j in range(tp)
    ]
    gathered = [lax.ppermute(piece, ("kv", "tp"), pairs)]
    r = tp // 2
    at = [0]
    while r:
        gathered += [to_tp(x, r) for x in gathered]
        at += [s ^ r for s in at]
        r //= 2
    gathered = held_in_vmem([gathered[at.index(s)] for s in range(tp)])

    depth = 2 * size + rows + AUX
    packed = call(
        functools.partial(pack_kernel, heads, each),
        2,
        6,
        [pltpu.VMEM((each, depth, rows), BF16)] * kv,
        [pltpu.VMEM((heads, depth, rows), BF16)],
        None,
    )(me, block_picks, queries, keys, values, cotangent, attended, log_totals)
    msgs = held_in_vmem([packed[0]] + [to_kv(packed[r], r) for r in range(1, kv)])

    ext = LANES * (-(-(blocks + AUX) // LANES))
    total = kv * rows
    sent = call(
        functools.partial(head_kernel, group, blocks, slots),
        1,
        kv,
        [pltpu.VMEM((each, kv * size + rows, LANES), BF16)] * group,
        [
            pltpu.VMEM((each, total, LANES + ext), BF16),
            pltpu.VMEM((each, size, total), BF16),
            pltpu.VMEM((each, 2, LANES + ext, total), BF16),
            pltpu.VMEM((each, total, LANES), F32),
            pltpu.VMEM((each, size, total), BF16),
        ],
    )(me, *msgs)
    gots = held_in_vmem([sent[0]] + [to_kv(sent[r], r) for r in range(1, group)])

    return call(
        functools.partial(final_kernel, group, tp),
        2,
        group + tp,
        [jax.ShapeDtypeStruct((rows, width), BF16)] * 3 + [jax.ShapeDtypeStruct((part, width), F32)],
        [
            pltpu.VMEM((tp, heads * size, total // tp), BF16),
            pltpu.VMEM((heads, rows, LANES), BF16),
        ],
    )(me, mine_tp, *gots, *gathered)


def solution(mesh):
    in_specs = (
        P("kv", "tp"),
        P("kv", "tp"),
        P("kv", "tp"),
        P("kv", "tp"),
        P("kv", "tp"),
        P("tp", "kv"),
        P("tp", "kv", None),
        P("kv", "tp"),
    )
    out_specs = (P("kv", "tp"), P("kv", "tp"), P("kv", "tp"), P("kv", "tp"))

    def step(*args):
        return tuple(local(*args))

    step = jax.shard_map(step, mesh=mesh, in_specs=in_specs, out_specs=out_specs, check_vma=False)
    return step
```
